32 devices in a mesh: grp: 2 (over y), fs: 4 (over z), tp: 4 (over x, core).
Axes of the slice: x: 2, y: 2, z: 4, core: 2. Of those that a mesh axis runs over, the one named last changes fastest.
Arguments:
- tokens: bfloat16 [1024, 2048], P(('grp', 'fs'), 'tp'), parts along dimension 0, may hold values from -300 to 300
- routes: int32 [1024, 2], P(('grp', 'fs')), parts along dimension 0, may hold values from 0 to 3, all different within a row; in each aligned block of 128 rows (0 to 127, 128 to 255, ...) at most 128 rows name the same one
- route_scores: float32 [1024, 2], P(('grp', 'fs')), parts along dimension 0, may hold values from 0.05 to 1
- norm_gain: float32 [2048], P('fs'), may hold values from 0.1 to 1.9
- expert_gate: float32 [4, 2048, 256], P(None, 'fs', 'tp'), may hold values from -6 to 6
- expert_up: float32 [4, 2048, 256], P(None, 'fs', 'tp'), may hold values from -6 to 6
- expert_down: float32 [4, 2048, 256], P(None, 'fs', 'tp'), may hold values from -6 to 6
- shared_gate: float32 [2048, 256], P('fs', 'tp'), may hold values from -6 to 6
- shared_up: float32 [2048, 256], P('fs', 'tp'), may hold values from -6 to 6
- shared_down: float32 [2048, 256], P('fs', 'tp'), may hold values from -6 to 6
Outputs:
- served_gate: bfloat16 [8, 2048, 256], P(('grp', 'fs'), 'tp'), parts along dimension 0
- served_up: bfloat16 [8, 2048, 256], P(('grp', 'fs'), 'tp'), parts along dimension 0
- served_down: bfloat16 [8, 2048, 256], P(('grp', 'fs'), 'tp'), parts along dimension 0
- common_gate: bfloat16 [4096, 256], P(('grp', 'tp')), parts along dimension 0
- common_up: bfloat16 [4096, 256], P(('grp', 'tp')), parts along dimension 0
- common_down: bfloat16 [4096, 256], P(('grp', 'tp')), parts along dimension 0
- mixture: bfloat16 [1024, 2048], P(('grp', 'fs'), 'tp'), parts along dimension 0
The draws below stay inside these ranges and needn't reach their ends.
There are 2 independent parts, one for each index of `grp`. The reference program is written for one: setup_inputs(seed, part) draws one part's arguments, and reference() takes and returns one part's arrays. A program takes and returns all parts, laid end to end along the dimension named above; an argument that names none is the same for every part. Nothing has to cross between parts.
Inputs may be any that keep to these rules, and one draw needn't show every extreme that they name: `routes`: each row names 2 different experts. Within the rows of one index of fs (aligned blocks of 128 rows) no expert is named by more than 128 rows, a bound that some block reaches.
All inputs are finite; a program needn't handle non-finite values.
Results may differ from the reference program's by a relative error of at most 0.018.
Values may be sent and summed in bfloat16 or wider, within the bound.
A program may use at most 64 MiB of HBM per device.

```python
import math
import jax
import jax.numpy as jnp
import numpy as np
from jax import lax

D = 2048
H = 256
SH = 256
TOK_DEV = 128
TOKENS = 512
EXPERTS = 4
TOP_K = 2
CAP = 128
N_FS = 4
N_TP = 4


def draw_tokens(key, part):
    base_key = jax.random.fold_in(key, 11)
    subkeys = jax.random.split(base_key, 2)
    column_scale = jnp.exp(math.log(3.0) * jnp.arange(D, dtype=jnp.float32) / D)
    column_scale = column_scale * jax.random.uniform(subkeys[1], (D,), jnp.float32, 0.5, 1.5)
    values = jnp.clip(jax.random.normal(subkeys[0], (TOKENS, D), jnp.float32), -6.0, 6.0)
    return (values * column_scale[None, :]).astype(jnp.bfloat16)


def block_scale(key, shape, cuts, least, high):
    factor_of, own = 1.0, jax.random.fold_in(key, 6)
    for position, parts in cuts:
        heights = jnp.exp(jax.random.uniform(jax.random.fold_in(own, position), (parts,), jnp.float32, least / len(cuts), high / len(cuts)))
        factor_of = factor_of * jnp.repeat(heights, shape[position] // parts).reshape([-1 if axis == position else 1 for axis in range(len(shape))])
    return factor_of


def assign_block(stream_key, own, number, rows, count, top, most, skew):
    ranking = jax.random.permutation(stream_key, count)
    heavy_load, ordinary = portions_of(count, rows * top, most, skew, True), portions_of(count, rows * top, most, skew, False)
    places = jnp.arange(count)

    def named(lengths, turn):
        used = int((lengths > 0).sum())
        fixed = max(1, used // 4)
        passed = fixed + (places - fixed + turn * (used - fixed)) % max(1, count - fixed)
        return jnp.zeros((count,), jnp.int32).at[ranking[jnp.where(places < fixed, places, passed)]].set(jnp.asarray(lengths, jnp.int32))

    lengths = jnp.where(number % 4 == 0, named(heavy_load, number // 4), named(ordinary, number - number // 4 - 1))
    mixed = jax.random.permutation(jax.random.fold_in(own, 3), count)
    donor, sink = mixed[0:count // 2 * 2:2], mixed[1:count // 2 * 2:2]
    margin = jnp.minimum(lengths[donor] - 1, most - lengths[sink]) // 2
    margin = jnp.where((donor == ranking[0]) | (sink == ranking[0]) | (lengths[sink] == 0), 0, jnp.maximum(margin, 0))
    passed = jax.random.randint(jax.random.fold_in(own, 4), (count // 2,), 0, 1 << 20) % (margin + 1)
    lengths = lengths.at[donor].add(-passed).at[sink].add(passed)
    labels = jnp.searchsorted(jnp.cumsum(lengths), jnp.arange(rows * top), side="right").astype(jnp.int32)
    grid = labels.reshape(top, rows).T
    grid = grid[jax.random.permutation(jax.random.fold_in(own, 1), rows)]
    turn = jax.random.randint(jax.random.fold_in(own, 2), (rows, 1), 0, top)
    return jnp.take_along_axis(grid, (jnp.arange(top)[None, :] + turn) % top, axis=1)


def portions_of(count, total, bound, slope, full):
    portions = [(1 << 20) // math.isqrt(rank ** slope) + 1 for rank in range(1, count + 1)]
    largest = bound if full else min(bound, max(-(-total // count), total * portions[0] // sum(portions)))
    least = 1 if total - largest >= count - 1 else 0
    holding, spare = [largest] + [least] * (count - 1), total - largest - least * (count - 1)
    while spare > 0:
        candidates = [i for i in range(1, count) if holding[i] < largest] or [i for i in range(1, count) if holding[i] < bound]
        whole, remaining = sum([portions[i] for i in candidates]), spare
        for i in candidates:
            addition = min(bound - holding[i], max(1, remaining * portions[i] // whole), spare)
            holding[i] = holding[i] + addition
            spare = spare - addition
    return np.array(holding)


def centred(stream_key, shape, deviation, reach, cuts=(), kind=jnp.bfloat16):
    entries = deviation * jax.random.normal(stream_key, shape, jnp.float32)
    if cuts:
        entries = entries * block_scale(stream_key, shape, cuts, -0.22, 0.18)
    return jnp.clip(entries, -reach, reach).astype(kind)


def setup_inputs(seed: int = 0, part: int = 0) -> dict:
    key_of = jax.random.split(jax.random.key(seed), 11)
    part_keys = jax.random.split(jax.random.fold_in(key_of[10], part), 11)
    tokens = draw_tokens(jax.random.fold_in(jax.random.fold_in(key_of[10], part), 71), part)
    routes_keys = jax.random.split(jax.random.fold_in(part_keys[1], 1), TOKENS // TOK_DEV)
    routes_turns = jax.random.permutation(jax.random.fold_in(part_keys[1], 3), TOKENS // TOK_DEV)
    routes = jax.vmap(lambda own, number: assign_block(jax.random.fold_in(part_keys[1], 2), own, number, TOK_DEV, EXPERTS, TOP_K, CAP, 1))(routes_keys, routes_turns).reshape((TOKENS, TOP_K))
    route_scores = jnp.clip(0.05 + 0.95 * jax.random.uniform(part_keys[2], (TOKENS, TOP_K), jnp.float32) ** block_scale(part_keys[2], (TOKENS, TOP_K), ((0, 4),), -0.2, 0.2), 0.05, 1.0)
    norm_gain = jnp.clip(1.0 + 0.18 * jax.random.normal(key_of[3], (D,), jnp.float32), 0.1, 1.9)
    expert_gate = centred(key_of[4], (EXPERTS, D, H), 1.0, 6.0, ((1, 4), (2, 4)), jnp.float32)
    expert_up = centred(key_of[5], (EXPERTS, D, H), 1.0, 6.0, ((1, 4), (2, 4)), jnp.float32)
    expert_down = centred(key_of[6], (EXPERTS, D, H), 1.0, 6.0, ((1, 4), (2, 4)), jnp.float32)
    shared_gate = centred(key_of[7], (D, SH), 1.0, 6.0, ((0, 4), (1, 4)), jnp.float32)
    shared_up = centred(key_of[8], (D, SH), 1.0, 6.0, ((0, 4), (1, 4)), jnp.float32)
    shared_down = centred(key_of[9], (D, SH), 1.0, 6.0, ((0, 4), (1, 4)), jnp.float32)
    return {"tokens": tokens, "routes": routes, "route_scores": route_scores, "norm_gain": norm_gain, "expert_gate": expert_gate, "expert_up": expert_up, "expert_down": expert_down, "shared_gate": shared_gate, "shared_up": shared_up, "shared_down": shared_down}


EPSILON = 1e-05
ROUTED_SCALE = 2.5

def normalize(tokens):
    values = tokens.astype(jnp.float32)
    average = lax.optimization_barrier(jnp.mean(values, axis=1, keepdims=True))
    meansq = lax.optimization_barrier(jnp.mean(values * values, axis=1, keepdims=True))
    return ((values - average) * lax.rsqrt(meansq - average * average + EPSILON)).astype(jnp.bfloat16)

def gated_mlp(inputs, w_gate, w_up, w_down):
    model_width = inputs.shape[1]
    block_width = model_width // N_TP
    hidden_units = w_gate.shape[1]
    gate_total = jnp.zeros((inputs.shape[0], hidden_units), jnp.float32)
    up_total = jnp.zeros((inputs.shape[0], hidden_units), jnp.float32)
    for block_index in range(N_TP):
        low = block_index * block_width
        columns = inputs[:, low:low + block_width]
        gate_piece = jnp.dot(columns, w_gate[low:low + block_width], preferred_element_type=jnp.float32) * model_width ** (-0.5)
        up_piece = jnp.dot(columns, w_up[low:low + block_width], preferred_element_type=jnp.float32) * model_width ** (-0.5)
        gate_total = gate_total + gate_piece.astype(jnp.bfloat16).astype(jnp.float32)
        up_total = up_total + up_piece.astype(jnp.bfloat16).astype(jnp.float32)
    hidden = (jax.nn.silu(gate_total) * up_total).astype(jnp.bfloat16)
    return jnp.dot(hidden, w_down.T, preferred_element_type=jnp.float32) * hidden_units ** (-0.5)

def reference(tokens, routes, route_scores, norm_gain, expert_gate, expert_up, expert_down, shared_gate, shared_up, shared_down):
    gain_column = norm_gain[:, None]
    served_gate = (expert_gate * gain_column[None]).astype(jnp.bfloat16)
    served_up = (expert_up * gain_column[None]).astype(jnp.bfloat16)
    served_down = expert_down.astype(jnp.bfloat16)
    common_gate = (shared_gate * gain_column).astype(jnp.bfloat16)
    common_up = (shared_up * gain_column).astype(jnp.bfloat16)
    common_down = shared_down.astype(jnp.bfloat16)
    normed = normalize(tokens)
    mix_weight = route_scores / lax.optimization_barrier(jnp.sum(route_scores, axis=1, keepdims=True)) * ROUTED_SCALE
    running = gated_mlp(normed, common_gate, common_up, common_down)
    expert_ids = routes.reshape(-1).astype(jnp.int32)
    count_all = expert_ids.shape[0]
    sorted_order = jnp.argsort(expert_ids, stable=True).astype(jnp.int32)
    counts = jax.ops.segment_sum(jnp.ones_like(expert_ids), expert_ids, num_segments=EXPERTS)
    starts = jnp.cumsum(counts) - counts
    most_rows = N_FS * CAP
    flat_weights = mix_weight.reshape(-1)

    def one_expert(carried, expert_index):
        offsets = jnp.arange(most_rows, dtype=jnp.int32)
        picked = sorted_order[jnp.minimum(starts[expert_index] + offsets, count_all - 1)]
        live_rows = offsets < counts[expert_index]
        token_ids = picked // TOP_K
        expert_out = gated_mlp(normed[token_ids], served_gate[expert_index], served_up[expert_index], served_down[expert_index])
        expert_out = expert_out.astype(jnp.bfloat16).astype(jnp.float32)
        row_weight = jnp.where(live_rows, flat_weights[picked], jnp.zeros_like(flat_weights[picked]))
        return (carried.at[token_ids].add(expert_out * row_weight[:, None]), None)
    running, _ = lax.scan(one_expert, running, jnp.arange(EXPERTS, dtype=jnp.int32))
    mixture = running.astype(jnp.bfloat16)
    return (served_gate, served_up, served_down, common_gate, common_up, common_down, mixture)
```

```python
import functools

import jax
import jax.numpy as jnp
from jax import lax
from jax.experimental import pallas as pl
from jax.experimental.pallas import tpu as pltpu
from jax.sharding import PartitionSpec as P

LANES = 128
EPSILON = 1e-05
ROUTED_SCALE = 2.5


def on_device(
    model_width,
    hidden_units,
    shared_units,
    tokens,
    routes,
    route_scores,
    norm_gain,
    expert_gate,
    expert_up,
    expert_down,
    shared_gate,
    shared_up,
    shared_down,
):
    D, H, SH = model_width, hidden_units, shared_units
    gain_column = norm_gain[:, None]
    gate_rows, up_rows, down_rows = (
        lax.all_to_all(
            (expert_gate * gain_column[None]).astype(jnp.bfloat16),
            "fs",
            split_axis=0,
            concat_axis=1,
            tiled=True,
        ),
        lax.all_to_all(
            (expert_up * gain_column[None]).astype(jnp.bfloat16),
            "fs",
            split_axis=0,
            concat_axis=1,
            tiled=True,
        ),
        lax.all_to_all(
            expert_down.astype(jnp.bfloat16), "fs", split_axis=0, concat_axis=1, tiled=True
        ),
    )
    shared_gate_rows, shared_up_rows, shared_down_rows = (
        lax.all_gather((shared_gate * gain_column).astype(jnp.bfloat16), "fs", axis=0, tiled=True),
        lax.all_gather((shared_up * gain_column).astype(jnp.bfloat16), "fs", axis=0, tiled=True),
        lax.all_gather(shared_down.astype(jnp.bfloat16), "fs", axis=0, tiled=True),
    )
    served_gate, served_up, served_down, common_gate, common_up, common_down = (
        lax.all_to_all(gate_rows[0], "tp", split_axis=0, concat_axis=1, tiled=True),
        lax.all_to_all(up_rows[0], "tp", split_axis=0, concat_axis=1, tiled=True),
        lax.all_to_all(down_rows[0], "tp", split_axis=0, concat_axis=1, tiled=True),
        lax.all_to_all(shared_gate_rows, "tp", split_axis=0, concat_axis=1, tiled=True),
        lax.all_to_all(shared_up_rows, "tp", split_axis=0, concat_axis=1, tiled=True),
        lax.all_to_all(shared_down_rows, "tp", split_axis=0, concat_axis=1, tiled=True),
    )
    values = tokens.astype(jnp.float32)
    feature_sum, square_sum = lax.psum(
        (jnp.sum(values, axis=1), jnp.sum(values * values, axis=1)), "tp"
    )
    average = feature_sum / D
    variance = square_sum / D - average * average
    normed = ((values - average[:, None]) * lax.rsqrt(variance + EPSILON)[:, None]).astype(
        jnp.bfloat16
    )
    shared_gate_part = jnp.dot(normed, common_gate, preferred_element_type=jnp.float32) * D ** (
        -0.5
    )
    shared_up_part = jnp.dot(normed, common_up, preferred_element_type=jnp.float32) * D ** (-0.5)
    shared_gate_total, shared_up_total = (
        lax.psum(shared_gate_part.astype(jnp.bfloat16), "tp").astype(jnp.float32),
        lax.psum(shared_up_part.astype(jnp.bfloat16), "tp").astype(jnp.float32),
    )
    shared_hidden = (jax.nn.silu(shared_gate_total) * shared_up_total).astype(jnp.bfloat16)
    shared_part = jnp.einsum(
        "th,dh->td", shared_hidden, common_down, preferred_element_type=jnp.float32
    ) * SH ** (-0.5)
    tok_rows, top_count = routes.shape
    experts = expert_gate.shape[0]
    capacity = 2 * tok_rows * top_count // experts
    expert_ids = routes.reshape(-1)
    one_hot = (expert_ids[:, None] == jnp.arange(experts, dtype=jnp.int32)[None, :]).astype(
        jnp.int32
    )
    slot_rank = jnp.sum(jnp.cumsum(one_hot, axis=0) * one_hot, axis=1) - 1
    slot_index = expert_ids * capacity + slot_rank
    token_index = jnp.arange(expert_ids.shape[0], dtype=jnp.int32) // top_count
    slot_token = (
        jnp.full((experts * capacity,), tok_rows, jnp.int32).at[slot_index].set(token_index)
    )
    padded = jnp.concatenate([normed, jnp.zeros((1, normed.shape[1]), jnp.bfloat16)], axis=0)
    outgoing = padded[slot_token].reshape(experts, capacity, normed.shape[1])
    received = lax.all_to_all(outgoing, "fs", split_axis=0, concat_axis=0, tiled=True)
    gate_part = jnp.einsum(
        "scd,dh->sch", received, served_gate, preferred_element_type=jnp.float32
    ) * D ** (-0.5)
    up_part = jnp.einsum(
        "scd,dh->sch", received, served_up, preferred_element_type=jnp.float32
    ) * D ** (-0.5)
    gate_total = lax.psum(gate_part.astype(jnp.bfloat16), "tp").astype(jnp.float32)
    up_total = lax.psum(up_part.astype(jnp.bfloat16), "tp").astype(jnp.float32)
    hidden = (jax.nn.silu(gate_total) * up_total).astype(jnp.bfloat16)
    expert_out = jnp.einsum(
        "sch,dh->scd", hidden, served_down, preferred_element_type=jnp.float32
    ) * H ** (-0.5)
    returned = lax.all_to_all(
        expert_out.astype(jnp.bfloat16), "fs", split_axis=0, concat_axis=0, tiled=True
    )
    picked = returned.reshape(experts * capacity, returned.shape[2])[slot_index]
    picked = picked.reshape(tok_rows, top_count, returned.shape[2]).astype(jnp.float32)
    mix_weight = route_scores / jnp.sum(route_scores, axis=1, keepdims=True) * ROUTED_SCALE
    routed_part = jnp.sum(picked * mix_weight[:, :, None], axis=1)
    mixture = (shared_part + routed_part).astype(jnp.bfloat16)
    return (
        served_gate[None],
        served_up[None],
        served_down[None],
        common_gate,
        common_up,
        common_down,
        mixture,
    )


def fused_kernel(
    G, F, T, D, H,
    tok, routes, scores, gain, eg, eu, ed, sg, su, sd,
    o_sg, o_su, o_sd, o_cg, o_cu, o_cd, o_mix,
    w32, sendg, sendd, zg, zd, xg, xd, wfull, dfull,
    stat, tbuf, pbuf, rbuf, hbuf, obuf, ret,
    l_sem, zg_s, zg_r, zd_s, zd_r, xg_s, xg_r, xd_s, xd_r,
    st_s, st_r, tk_s, tk_r, rs_s, rs_r, ag_s, ag_r, rt_s, rt_r, out_sem,
):
    y, z, t = lax.axis_index("grp"), lax.axis_index("fs"), lax.axis_index("tp")
    E, Dz, Hs = eg.shape
    R, FD = tok.shape
    hr = Dz // G
    hd = hr // 2
    sr = R // T

    def at(y2, z2, t2):
        return {"grp": y2, "fs": z2, "tp": t2}

    def rc(src, dst, ss, rs, dev):
        return pltpu.make_async_remote_copy(
            src_ref=src, dst_ref=dst, send_sem=ss, recv_sem=rs,
            device_id=dev, device_id_type=pl.DeviceIdType.MESH,
        )

    half = pl.ds(pl.multiple_of(y * hr, hr), hr)
    loads = []
    for i, (ref, sref) in enumerate(((eg, sg), (eu, su), (ed, sd))):
        loads.append(pltpu.make_async_copy(ref.at[:, half, :], w32.at[i, pl.ds(0, E)], l_sem.at[2 * i]))
        loads.append(pltpu.make_async_copy(sref.at[half, :], w32.at[i, E], l_sem.at[2 * i + 1]))
    for c in loads:
        c.start()

    barrier = pltpu.get_barrier_semaphore()
    peers = [at(y, lax.rem(z + d, F), t) for d in range(1, F)]
    for dy in range(G):
        for dt in range(T):
            if dy or dt:
                peers.append(at(lax.rem(y + dy, G), z, lax.rem(t + dt, T)))
    for dev in peers:
        pl.semaphore_signal(barrier, inc=1, device_id=dev, device_id_type=pl.DeviceIdType.MESH)

    x = tok[...].astype(jnp.float32)
    s1 = jnp.sum(x, axis=1, keepdims=True)
    s2 = jnp.sum(x * x, axis=1, keepdims=True)
    lane = lax.broadcasted_iota(jnp.int32, (R, LANES), 1)
    stat[t] = jnp.where(lane == 0, s1, jnp.where(lane == 1, s2, 0.0)).T[0:8]
    gcol = jnp.concatenate(
        [
            jnp.broadcast_to(
                gain[0:1, pl.ds(pl.multiple_of(y * hr + i * LANES, LANES), LANES)], (LANES, LANES)
            ).T[:, 0:Hs]
            for i in range(hr // LANES)
        ],
        axis=0,
    )

    pl.semaphore_wait(barrier, len(peers))
    stat_copies = []
    for d in range(1, T):
        c = rc(stat.at[t], stat.at[t], st_s.at[d - 1], st_r.at[t], at(y, z, lax.rem(t + d, T)))
        c.start()
        stat_copies.append(c)

    for c in loads[:4]:
        c.wait()

    def pack_gu(e):
        return jnp.concatenate([w32[0, e] * gcol, w32[1, e] * gcol], axis=1).astype(jnp.bfloat16)

    def pack_d(e):
        return jnp.concatenate([w32[2, e, 0:hd], w32[2, e, hd:hr]], axis=1).astype(jnp.bfloat16)

    common = pack_gu(E)
    for e in range(E):
        sendg[e, 0] = pack_gu(e)
        sendg[e, 1] = common
    zg_copies = []
    for d in range(1, F):
        z2 = lax.rem(z + d, F)
        c = rc(sendg.at[z2], zg.at[z], zg_s.at[d - 1], zg_r.at[z], at(y, z2, t))
        c.start()
        zg_copies.append(c)
    pltpu.make_async_copy(sendg.at[z], zg.at[z], zg_r.at[z]).start()

    for d in range(1, T):
        t2 = lax.rem(t + d, T)
        rc(stat.at[t2], stat.at[t2], st_s.at[d - 1], st_r.at[t2], at(y, z, t2)).wait_recv()
    tot = stat[0]
    for i in range(1, T):
        tot = tot + stat[i]
    back = jnp.concatenate([tot, jnp.zeros((LANES - 8, R), jnp.float32)], axis=0).T
    average = back[:, 0:1] / D
    variance = back[:, 1:2] / D - average * average
    tbuf[z] = ((tok[...].astype(jnp.float32) - average) * lax.rsqrt(variance + EPSILON)).astype(jnp.bfloat16)
    tok_copies = []
    for d in range(1, F):
        c = rc(tbuf.at[z], tbuf.at[z], tk_s.at[d - 1], tk_r.at[z], at(y, lax.rem(z + d, F), t))
        c.start()
        tok_copies.append(c)

    for c in loads[4:]:
        c.wait()
    common_d = pack_d(E)
    for e in range(E):
        sendd[e, 0] = pack_d(e)
        sendd[e, 1] = common_d
    zd_copies = []
    for d in range(1, F):
        z2 = lax.rem(z + d, F)
        c = rc(sendd.at[z2], zd.at[z], zd_s.at[d - 1], zd_r.at[z], at(y, z2, t))
        c.start()
        zd_copies.append(c)
    pltpu.make_async_copy(sendd.at[z], zd.at[z], zd_r.at[z]).start()

    def forward(zb, xb, zr, xs, xr):
        waits = []
        for d in range(F):
            f = lax.rem(z + F - d, F)
            pltpu.make_async_copy(zb.at[f], zb.at[f], zr.at[f]).wait()
            for dy in range(G):
                c = rc(
                    zb.at[f], xb.at[y * T + t], xs.at[d * G + dy], xr.at[y * T + t],
                    at(lax.rem(y + dy, G), z, f),
                )
                if dy:
                    c.start()
                    waits.append((None, c))
                else:
                    other = f != t
                    pl.when(other)(c.start)
                    own = pltpu.make_async_copy(zb.at[f], xb.at[y * T + t], xr.at[y * T + t])
                    pl.when(f == t)(own.start)
                    waits.append((other, c))
        return waits

    def arrived(xb, xr):
        for s in range(G * T):
            pltpu.make_async_copy(xb.at[s], xb.at[s], xr.at[s]).wait()

    xg_waits = forward(zg, xg, zg_r, xg_s, xg_r)
    arrived(xg, xg_r)

    for k in range(2):
        for ys in range(G):
            for p in range(T // 2):
                a, b = xg[ys * T + 2 * p, k], xg[ys * T + 2 * p + 1, k]
                rows, cols = pl.ds(ys * hr, hr), pl.ds(p * LANES, LANES)
                wfull[k, rows, cols] = jnp.concatenate([a[:, :Hs], b[:, :Hs]], axis=1)
                wfull[k, rows, pl.ds(H + p * LANES, LANES)] = jnp.concatenate([a[:, Hs:], b[:, Hs:]], axis=1)
    outs = [
        pltpu.make_async_copy(wfull.at[0, :, pl.ds(0, H)], o_sg, out_sem.at[0]),
        pltpu.make_async_copy(wfull.at[0, :, pl.ds(H, H)], o_su, out_sem.at[1]),
        pltpu.make_async_copy(wfull.at[1, :, pl.ds(0, H)], o_cg, out_sem.at[2]),
        pltpu.make_async_copy(wfull.at[1, :, pl.ds(H, H)], o_cu, out_sem.at[3]),
    ]
    for c in outs:
        c.start()

    spart = (jnp.dot(tbuf[z], wfull[1], preferred_element_type=jnp.float32) * D ** (-0.5)).astype(jnp.bfloat16)
    for j in range(T):
        pbuf[j, R:R + sr] = spart[j * sr:(j + 1) * sr]
    for d in range(1, F):
        z2 = lax.rem(z + d, F)
        pltpu.make_async_copy(tbuf.at[z2], tbuf.at[z2], tk_r.at[z2]).wait()
    rs_copies = []
    for d in range(T):
        j = lax.rem(t + 1 + d, T)
        pbuf[j, 0:R] = (
            jnp.dot(tbuf[j], wfull[0], preferred_element_type=jnp.float32) * D ** (-0.5)
        ).astype(jnp.bfloat16)
        if d < T - 1:
            c = rc(pbuf.at[j], rbuf.at[t], rs_s.at[d], rs_r.at[t], at(y, z, j))
            c.start()
            rs_copies.append(c)

    xd_waits = forward(zd, xd, zd_r, xd_s, xd_r)

    acc = pbuf[t].astype(jnp.float32)
    for d in range(1, T):
        t2 = lax.rem(t + d, T)
        pltpu.make_async_copy(rbuf.at[t2], rbuf.at[t2], rs_r.at[t2]).wait()
        acc = acc + rbuf[t2].astype(jnp.float32)
    gate, up = acc[:, 0:H], acc[:, H:]
    hbuf[t] = (gate / (1.0 + jnp.exp(-gate)) * up).astype(jnp.bfloat16)
    ag_copies = []
    for d in range(1, T):
        c = rc(hbuf.at[t], hbuf.at[t], ag_s.at[d - 1], ag_r.at[t], at(y, z, lax.rem(t + d, T)))
        c.start()
        ag_copies.append(c)

    arrived(xd, xd_r)
    for k in range(2):
        for ys in range(G):
            for p in range(T // 2):
                a, b = xd[ys * T + 2 * p, k], xd[ys * T + 2 * p + 1, k]
                cols = pl.ds(p * LANES, LANES)
                dfull[k, pl.ds(ys * hr, hd), cols] = jnp.concatenate([a[:, :Hs], b[:, :Hs]], axis=1)
                dfull[k, pl.ds(ys * hr + hd, hd), cols] = jnp.concatenate([a[:, Hs:], b[:, Hs:]], axis=1)
    douts = [
        pltpu.make_async_copy(dfull.at[0], o_sd, out_sem.at[4]),
        pltpu.make_async_copy(dfull.at[1], o_cd, out_sem.at[5]),
    ]
    for c in douts:
        c.start()
    for d in range(1, T):
        t2 = lax.rem(t + d, T)
        pltpu.make_async_copy(hbuf.at[t2], hbuf.at[t2], ag_r.at[t2]).wait()

    def down(h, k):
        return lax.dot_general(
            h, dfull[k], (((1,), (1,)), ((), ())), preferred_element_type=jnp.float32
        ) * H ** (-0.5)

    rt_copies = []
    for d in range(1, F + 1):
        j = lax.rem(z + d, F)
        value = down(hbuf[j, 0:R], 0).astype(jnp.bfloat16)
        if d < F:
            obuf[j] = value
            c = rc(obuf.at[j], ret.at[z], rt_s.at[d - 1], rt_r.at[z], at(y, j, t))
            c.start()
            rt_copies.append(c)
        else:
            ret[z] = value
    total = down(jnp.concatenate([hbuf[j, R:R + sr] for j in range(T)], axis=0), 1)
    score_sum = jnp.sum(scores[...], axis=1, keepdims=True)
    K = routes.shape[1]
    weight = scores[...] / score_sum * ROUTED_SCALE
    picked = routes[...]
    for d in range(1, F):
        z2 = lax.rem(z + d, F)
        pltpu.make_async_copy(ret.at[z2], ret.at[z2], rt_r.at[z2]).wait()
    for e in range(E):
        share = jnp.sum(jnp.where(picked == e, weight, 0.0), axis=1, keepdims=True)
        total = total + share * ret[e].astype(jnp.float32)
    o_mix[...] = total.astype(jnp.bfloat16)

    for c in stat_copies + zg_copies + tok_copies + zd_copies + rs_copies + ag_copies + rt_copies:
        c.wait_send()
    for other, c in xg_waits + xd_waits:
        if other is None:
            c.wait_send()
        else:
            pl.when(other)(c.wait_send)
    for c in outs + douts:
        c.wait()


def fused(
    G, F, T,
    tokens, routes, route_scores, norm_gain,
    expert_gate, expert_up, expert_down, shared_gate, shared_up, shared_down,
):
    R, FD = tokens.shape
    E, Dz, Hs = expert_gate.shape
    D, H = FD * T, Hs * T
    hr = Dz // G
    hd = hr // 2
    sr = R // T
    bf, f32 = jnp.bfloat16, jnp.float32
    vm, hbm = pl.BlockSpec(memory_space=pltpu.VMEM), pl.BlockSpec(memory_space=pl.ANY)
    dma = lambda n: pltpu.SemaphoreType.DMA((n,))
    weights = jax.ShapeDtypeStruct((FD, H), bf)
    res = pl.pallas_call(
        functools.partial(fused_kernel, G, F, T, D, H),
        out_shape=[weights] * 6 + [jax.ShapeDtypeStruct((R, FD), bf)],
        in_specs=[vm] * 4 + [hbm] * 6,
        out_specs=[hbm] * 6 + [vm],
        scratch_shapes=[
            pltpu.VMEM((3, E + 1, hr, Hs), f32),
            pltpu.VMEM((E, 2, hr, LANES), bf),
            pltpu.VMEM((E, 2, hd, LANES), bf),
            pltpu.VMEM((F, 2, hr, LANES), bf),
            pltpu.VMEM((F, 2, hd, LANES), bf),
            pltpu.VMEM((G * T, 2, hr, LANES), bf),
            pltpu.VMEM((G * T, 2, hd, LANES), bf),
            pltpu.VMEM((2, FD, 2 * H), bf),
            pltpu.VMEM((2, FD, H), bf),
            pltpu.VMEM((T, 8, R), f32),
            pltpu.VMEM((F, R, FD), bf),
            pltpu.VMEM((T, R + sr, 2 * H), bf),
            pltpu.VMEM((T, R + sr, 2 * H), bf),
            pltpu.VMEM((T, R + sr, H), bf),
            pltpu.VMEM((F, R, FD), bf),
            pltpu.VMEM((F, R, FD), bf),
            dma(6), dma(F), dma(F), dma(F), dma(F),
            dma(F * G), dma(G * T), dma(F * G), dma(G * T),
            dma(T), dma(T), dma(F), dma(F), dma(T), dma(T), dma(T), dma(T), dma(F), dma(F), dma(6),
        ],
        compiler_params=pltpu.CompilerParams(collective_id=0, has_side_effects=True),
    )(
        tokens, routes, route_scores, norm_gain.reshape(1, Dz),
        expert_gate, expert_up, expert_down, shared_gate, shared_up, shared_down,
    )
    return tuple(r[None] for r in res[:3]) + tuple(res[3:])


def dispatch(
    G, F, T,
    tokens, routes, route_scores, norm_gain,
    expert_gate, expert_up, expert_down, shared_gate, shared_up, shared_down,
):
    R, FD = tokens.shape
    E, Dz, Hs = expert_gate.shape
    args = (
        tokens, routes, route_scores, norm_gain,
        expert_gate, expert_up, expert_down, shared_gate, shared_up, shared_down,
    )
    dense = (
        F == T and E == F and Dz == FD and 2 * Hs == LANES and R == LANES and T % 2 == 0
        and shared_gate.shape[1] == Hs and Dz % (2 * LANES * G) == 0 and R % (16 * T) == 0
        and 2 * R * routes.shape[1] >= E * R
    )
    if dense:
        return fused(G, F, T, *args)
    return on_device(FD * T, Hs * T, shared_gate.shape[1] * T, *args)


def solution(mesh):
    in_specs = (
        P(("grp", "fs"), "tp"),
        P(("grp", "fs"), None),
        P(("grp", "fs"), None),
        P("fs"),
        P(None, "fs", "tp"),
        P(None, "fs", "tp"),
        P(None, "fs", "tp"),
        P("fs", "tp"),
        P("fs", "tp"),
        P("fs", "tp"),
    )
    out_specs = (
        P(("grp", "fs"), "tp", None),
        P(("grp", "fs"), "tp", None),
        P(("grp", "fs"), "tp", None),
        P(("grp", "tp"), None),
        P(("grp", "tp"), None),
        P(("grp", "tp"), None),
        P(("grp", "fs"), "tp"),
    )
    return jax.shard_map(
        functools.partial(dispatch, mesh.shape["grp"], mesh.shape["fs"], mesh.shape["tp"]),
        mesh=mesh,
        in_specs=in_specs,
        out_specs=out_specs,
        check_vma=False,
    )
```

```python
import functools

import jax
import jax.numpy as jnp
from jax import lax
from jax.experimental import pallas as pl
from jax.experimental.pallas import tpu as pltpu
from jax.sharding import PartitionSpec as P

LANES = 128
EPSILON = 1e-05
ROUTED_SCALE = 2.5


def on_device(
    model_width,
    hidden_units,
    shared_units,
    tokens,
    routes,
    route_scores,
    norm_gain,
    expert_gate,
    expert_up,
    expert_down,
    shared_gate,
    shared_up,
    shared_down,
):
    D, H, SH = model_width, hidden_units, shared_units
    gain_column = norm_gain[:, None]
    gate_rows, up_rows, down_rows = (
        lax.all_to_all(
            (expert_gate * gain_column[None]).astype(jnp.bfloat16),
            "fs",
            split_axis=0,
            concat_axis=1,
            tiled=True,
        ),
        lax.all_to_all(
            (expert_up * gain_column[None]).astype(jnp.bfloat16),
            "fs",
            split_axis=0,
            concat_axis=1,
            tiled=True,
        ),
        lax.all_to_all(
            expert_down.astype(jnp.bfloat16), "fs", split_axis=0, concat_axis=1, tiled=True
        ),
    )
    shared_gate_rows, shared_up_rows, shared_down_rows = (
        lax.all_gather((shared_gate * gain_column).astype(jnp.bfloat16), "fs", axis=0, tiled=True),
        lax.all_gather((shared_up * gain_column).astype(jnp.bfloat16), "fs", axis=0, tiled=True),
        lax.all_gather(shared_down.astype(jnp.bfloat16), "fs", axis=0, tiled=True),
    )
    served_gate, served_up, served_down, common_gate, common_up, common_down = (
        lax.all_to_all(gate_rows[0], "tp", split_axis=0, concat_axis=1, tiled=True),
        lax.all_to_all(up_rows[0], "tp", split_axis=0, concat_axis=1, tiled=True),
        lax.all_to_all(down_rows[0], "tp", split_axis=0, concat_axis=1, tiled=True),
        lax.all_to_all(shared_gate_rows, "tp", split_axis=0, concat_axis=1, tiled=True),
        lax.all_to_all(shared_up_rows, "tp", split_axis=0, concat_axis=1, tiled=True),
        lax.all_to_all(shared_down_rows, "tp", split_axis=0, concat_axis=1, tiled=True),
    )
    values = tokens.astype(jnp.float32)
    feature_sum, square_sum = lax.psum(
        (jnp.sum(values, axis=1), jnp.sum(values * values, axis=1)), "tp"
    )
    average = feature_sum / D
    variance = square_sum / D - average * average
    normed = ((values - average[:, None]) * lax.rsqrt(variance + EPSILON)[:, None]).astype(
        jnp.bfloat16
    )
    shared_gate_part = jnp.dot(normed, common_gate, preferred_element_type=jnp.float32) * D ** (
        -0.5
    )
    shared_up_part = jnp.dot(normed, common_up, preferred_element_type=jnp.float32) * D ** (-0.5)
    shared_gate_total, shared_up_total = (
        lax.psum(shared_gate_part.astype(jnp.bfloat16), "tp").astype(jnp.float32),
        lax.psum(shared_up_part.astype(jnp.bfloat16), "tp").astype(jnp.float32),
    )
    shared_hidden = (jax.nn.silu(shared_gate_total) * shared_up_total).astype(jnp.bfloat16)
    shared_part = jnp.einsum(
        "th,dh->td", shared_hidden, common_down, preferred_element_type=jnp.float32
    ) * SH ** (-0.5)
    tok_rows, top_count = routes.shape
    experts = expert_gate.shape[0]
    capacity = 2 * tok_rows * top_count // experts
    expert_ids = routes.reshape(-1)
    one_hot = (expert_ids[:, None] == jnp.arange(experts, dtype=jnp.int32)[None, :]).astype(
        jnp.int32
    )
    slot_rank = jnp.sum(jnp.cumsum(one_hot, axis=0) * one_hot, axis=1) - 1
    slot_index = expert_ids * capacity + slot_rank
    token_index = jnp.arange(expert_ids.shape[0], dtype=jnp.int32) // top_count
    slot_token = (
        jnp.full((experts * capacity,), tok_rows, jnp.int32).at[slot_index].set(token_index)
    )
    padded = jnp.concatenate([normed, jnp.zeros((1, normed.shape[1]), jnp.bfloat16)], axis=0)
    outgoing = padded[slot_token].reshape(experts, capacity, normed.shape[1])
    received = lax.all_to_all(outgoing, "fs", split_axis=0, concat_axis=0, tiled=True)
    gate_part = jnp.einsum(
        "scd,dh->sch", received, served_gate, preferred_element_type=jnp.float32
    ) * D ** (-0.5)
    up_part = jnp.einsum(
        "scd,dh->sch", received, served_up, preferred_element_type=jnp.float32
    ) * D ** (-0.5)
    gate_total = lax.psum(gate_part.astype(jnp.bfloat16), "tp").astype(jnp.float32)
    up_total = lax.psum(up_part.astype(jnp.bfloat16), "tp").astype(jnp.float32)
    hidden = (jax.nn.silu(gate_total) * up_total).astype(jnp.bfloat16)
    expert_out = jnp.einsum(
        "sch,dh->scd", hidden, served_down, preferred_element_type=jnp.float32
    ) * H ** (-0.5)
    returned = lax.all_to_all(
        expert_out.astype(jnp.bfloat16), "fs", split_axis=0, concat_axis=0, tiled=True
    )
    picked = returned.reshape(experts * capacity, returned.shape[2])[slot_index]
    picked = picked.reshape(tok_rows, top_count, returned.shape[2]).astype(jnp.float32)
    mix_weight = route_scores / jnp.sum(route_scores, axis=1, keepdims=True) * ROUTED_SCALE
    routed_part = jnp.sum(picked * mix_weight[:, :, None], axis=1)
    mixture = (shared_part + routed_part).astype(jnp.bfloat16)
    return (
        served_gate[None],
        served_up[None],
        served_down[None],
        common_gate,
        common_up,
        common_down,
        mixture,
    )


def fused_kernel(
    G, F, T, D, H,
    tok, routes, scores, gain, eg, eu, ed, sg, su, sd,
    o_sg, o_su, o_sd, o_cg, o_cu, o_cd, o_mix,
    w32, sendg, sendd, sends, zg, zd, zs, we, de, ws,
    stat, tbuf, pbuf, rbuf, hbuf, obuf, ret,
    l_sem, zg_s, zg_r, zd_s, zd_r, zs_s, zs_r, xg_s, xg_r, xd_s, xd_r, xs_s, xs_r,
    st_s, st_r, tk_s, tk_r, rs_s, rs_r, ag_s, ag_r, rt_s, rt_r,
):
    y, z, t = lax.axis_index("grp"), lax.axis_index("fs"), lax.axis_index("tp")
    E, Hs, Dz = eg.shape
    R, FD = tok.shape
    hr = Dz // G
    sr = R // T
    bf, f32 = jnp.bfloat16, jnp.float32

    def at(y2, z2, t2):
        return {"grp": y2, "fs": z2, "tp": t2}

    def rc(src, dst, ss, rs, dev):
        return pltpu.make_async_remote_copy(
            src_ref=src, dst_ref=dst, send_sem=ss, recv_sem=rs,
            device_id=dev, device_id_type=pl.DeviceIdType.MESH,
        )

    half = pl.ds(pl.multiple_of(y * hr, hr), hr)
    loads = []
    for i, (ref, sref) in enumerate(((eg, sg), (eu, su), (ed, sd))):
        loads.append(pltpu.make_async_copy(ref.at[:, :, half], w32.at[i, pl.ds(0, E)], l_sem.at[2 * i]))
        loads.append(pltpu.make_async_copy(sref.at[:, half], w32.at[i, E], l_sem.at[2 * i + 1]))
    loads = [loads[0], loads[2], loads[4], loads[1], loads[3], loads[5]]
    for c in loads:
        c.start()

    barrier = pltpu.get_barrier_semaphore()
    peers = [at(y, lax.rem(z + d, F), t) for d in range(1, F)]
    for dy in range(G):
        for dt in range(T):
            if dy or dt:
                peers.append(at(lax.rem(y + dy, G), z, lax.rem(t + dt, T)))
    for dev in peers:
        pl.semaphore_signal(barrier, inc=1, device_id=dev, device_id_type=pl.DeviceIdType.MESH)

    x = tok[...].astype(f32)
    s1 = jnp.sum(x, axis=1, keepdims=True)
    s2 = jnp.sum(x * x, axis=1, keepdims=True)
    lane = lax.broadcasted_iota(jnp.int32, (R, LANES), 1)
    stat[t] = jnp.where(lane == 0, s1, jnp.where(lane == 1, s2, 0.0)).T[0:8]
    gain_row = gain[0:1, half]

    loads[0].wait()
    loads[1].wait()
    for e in range(E):
        sendg[e, 0] = (w32[0, e] * gain_row).astype(bf)
        sendg[e, 1] = (w32[1, e] * gain_row).astype(bf)

    pl.semaphore_wait(barrier, len(peers))
    sent = []
    for d in range(1, T):
        c = rc(stat.at[t], stat.at[t], st_s.at[d - 1], st_r.at[t], at(y, z, lax.rem(t + d, T)))
        c.start()
        sent.append(c)

    def spread(src_of, zb, ss, rr):
        for d in range(1, F):
            z2 = lax.rem(z + d, F)
            c = rc(src_of(z2), zb.at[z], ss.at[d - 1], rr.at[z], at(y, z2, t))
            c.start()
            sent.append(c)
        pltpu.make_async_copy(src_of(z), zb.at[z], rr.at[z]).start()

    spread(lambda e: sendg.at[e], zg, zg_s, zg_r)

    for d in range(1, T):
        t2 = lax.rem(t + d, T)
        pltpu.make_async_copy(stat.at[t2], stat.at[t2], st_r.at[t2]).wait()
    tot = stat[0]
    for i in range(1, T):
        tot = tot + stat[i]
    back = jnp.concatenate([tot, jnp.zeros((LANES - 8, R), f32)], axis=0).T
    average = back[:, 0:1] / D
    variance = back[:, 1:2] / D - average * average
    tbuf[z] = ((tok[...].astype(f32) - average) * lax.rsqrt(variance + EPSILON)).astype(bf)
    for d in range(1, F):
        c = rc(tbuf.at[z], tbuf.at[z], tk_s.at[d - 1], tk_r.at[z], at(y, lax.rem(z + d, F), t))
        c.start()
        sent.append(c)

    for c in loads[2:]:
        c.wait()
    for e in range(E):
        sendd[e] = w32[2, e].astype(bf)
    spread(lambda e: sendd.at[e], zd, zd_s, zd_r)
    sends[0] = (w32[0, E] * gain_row).astype(bf)
    sends[1] = (w32[1, E] * gain_row).astype(bf)
    sends[2] = w32[2, E].astype(bf)
    spread(lambda e: sends, zs, zs_s, zs_r)

    held = []

    def forward(zb, place, zr, xs, xr):
        for d in range(F):
            f = lax.rem(z + F - d, F)
            pltpu.make_async_copy(zb.at[f], zb.at[f], zr.at[f]).wait()
            for dy in range(G):
                c = rc(
                    zb.at[f], place(y, t), xs.at[d * G + dy], xr.at[y * T + t],
                    at(lax.rem(y + dy, G), z, f),
                )
                if dy:
                    c.start()
                    sent.append(c)
                else:
                    own = pltpu.make_async_copy(zb.at[f], place(y, t), xr.at[y * T + t])
                    pl.when(f != t)(c.start)
                    pl.when(f == t)(own.start)
                    held.append((f != t, c))

    def arrived(place, xr):
        for ys in range(G):
            for tt in range(T):
                pltpu.make_async_copy(place(ys, tt), place(ys, tt), xr.at[ys * T + tt]).wait()

    def columns(ys):
        return pl.ds(pl.multiple_of(ys * hr, hr), hr)

    def at_e(ys, tt):
        return we.at[:, tt, :, columns(ys)]

    def at_d(ys, tt):
        return de.at[tt, :, columns(ys)]

    def at_s(ys, tt):
        return ws.at[:, tt, :, columns(ys)]

    def rows_of(i):
        return pl.ds(pl.multiple_of(i * sr, sr), sr)

    def first(s):
        if 0 < s < F:
            j = lax.rem(z + F - s, F)
            pltpu.make_async_copy(tbuf.at[j], tbuf.at[j], tk_r.at[j]).wait()
        else:
            j = z
        w = we[...] if s < F else ws[0:2]
        pbuf[s] = (
            lax.dot_general(
                tbuf[j], w.reshape(2 * H, FD), (((1,), (1,)), ((), ())), preferred_element_type=f32
            ) * D ** (-0.5)
        ).astype(bf)
        for d in range(1, T):
            t2 = lax.rem(t + d, T)
            c = rc(pbuf.at[s, rows_of(t2)], rbuf.at[s, t], rs_s.at[s * T + d], rs_r.at[s * T + t], at(y, z, t2))
            c.start()
            sent.append(c)

    def second(s):
        acc = pbuf[s, rows_of(t)].astype(f32)
        for d in range(1, T):
            t2 = lax.rem(t + d, T)
            pltpu.make_async_copy(rbuf.at[s, t2], rbuf.at[s, t2], rs_r.at[s * T + t2]).wait()
            acc = acc + rbuf[s, t2].astype(f32)
        gate, up = acc[:, 0:H], acc[:, H:]
        mine = hbuf.at[s, rows_of(t)]
        mine[...] = (gate / (1.0 + jnp.exp(-gate)) * up).astype(bf)
        for d in range(1, T):
            c = rc(mine, mine, ag_s.at[s * T + d], ag_r.at[s * T + t], at(y, z, lax.rem(t + d, T)))
            c.start()
            sent.append(c)

    def third(s):
        for d in range(1, T):
            t2 = lax.rem(t + d, T)
            theirs = hbuf.at[s, rows_of(t2)]
            pltpu.make_async_copy(theirs, theirs, ag_r.at[s * T + t2]).wait()
        w = de[...] if s < F else ws[2]
        value = jnp.dot(hbuf[s], w.reshape(H, FD), preferred_element_type=f32) * H ** (-0.5)
        if s == F:
            return value
        if s == 0:
            ret[z] = value.astype(bf)
        else:
            obuf[s] = value.astype(bf)
            c = rc(obuf.at[s], ret.at[z], rt_s.at[s], rt_r.at[z], at(y, lax.rem(z + F - s, F), t))
            c.start()
            sent.append(c)

    forward(zg, at_e, zg_r, xg_s, xg_r)
    arrived(at_e, xg_r)
    first(0)
    for s in range(1, F):
        first(s)
        second(s - 1)
    second(F - 1)
    forward(zd, at_d, zd_r, xd_s, xd_r)
    arrived(at_d, xd_r)
    for s in range(F):
        third(s)
    o_sg[...] = we[0].reshape(H, FD).T
    o_su[...] = we[1].reshape(H, FD).T
    o_sd[...] = de[...].reshape(H, FD).T
    forward(zs, at_s, zs_r, xs_s, xs_r)
    arrived(at_s, xs_r)
    first(F)
    o_cg[...] = ws[0].reshape(H, FD).T
    second(F)
    o_cu[...] = ws[1].reshape(H, FD).T
    o_cd[...] = ws[2].reshape(H, FD).T

    weight = scores[...] / jnp.sum(scores[...], axis=0, keepdims=True) * ROUTED_SCALE
    picked = routes[...]
    line = lax.broadcasted_iota(jnp.int32, (LANES, R), 0)
    shares = jnp.zeros((LANES, R), f32)
    for e in range(E):
        share = jnp.sum(jnp.where(picked == e, weight, 0.0), axis=0, keepdims=True)
        shares = jnp.where(line == e, share, shares)
    shares = shares.T
    total = third(F)
    for d in range(1, F):
        z2 = lax.rem(z + d, F)
        pltpu.make_async_copy(ret.at[z2], ret.at[z2], rt_r.at[z2]).wait()
    for e in range(E):
        total = total + shares[:, e:e + 1] * ret[e].astype(f32)
    o_mix[...] = total.astype(bf)

    for c in sent:
        c.wait_send()
    for other, c in held:
        pl.when(other)(c.wait_send)


def write_kernel(*refs):
    count = (len(refs) - 1) // 2
    sems = refs[-1]
    copies = [pltpu.make_async_copy(refs[i], refs[count + i], sems.at[i]) for i in range(count)]
    for c in copies:
        c.start()
    for c in copies:
        c.wait()


def fused(
    G, F, T,
    tokens, routes, route_scores, norm_gain,
    expert_gate, expert_up, expert_down, shared_gate, shared_up, shared_down,
):
    R, FD = tokens.shape
    E, Dz, Hs = expert_gate.shape
    D, H = FD * T, Hs * T
    hr = Dz // G
    sr = R // T
    B = F + 1
    bf, f32 = jnp.bfloat16, jnp.float32
    vm, hbm = pl.BlockSpec(memory_space=pltpu.VMEM), pl.BlockSpec(memory_space=pl.ANY)
    dma = lambda n: pltpu.SemaphoreType.DMA((n,))
    weights = jax.ShapeDtypeStruct((FD, H), bf)
    shapes = [weights] * 6 + [jax.ShapeDtypeStruct((R, FD), bf)]
    res = pl.pallas_call(
        functools.partial(fused_kernel, G, F, T, D, H),
        out_shape=shapes,
        in_specs=[vm] * 4 + [hbm] * 6,
        out_specs=[vm] * 7,
        scratch_shapes=[
            pltpu.VMEM((3, E + 1, Hs, hr), f32),
            pltpu.VMEM((E, 2, Hs, hr), bf),
            pltpu.VMEM((E, Hs, hr), bf),
            pltpu.VMEM((3, Hs, hr), bf),
            pltpu.VMEM((F, 2, Hs, hr), bf),
            pltpu.VMEM((F, Hs, hr), bf),
            pltpu.VMEM((F, 3, Hs, hr), bf),
            pltpu.VMEM((2, T, Hs, FD), bf),
            pltpu.VMEM((T, Hs, FD), bf),
            pltpu.VMEM((3, T, Hs, FD), bf),
            pltpu.VMEM((T, 8, R), f32),
            pltpu.VMEM((F, R, FD), bf),
            pltpu.VMEM((B, R, 2 * H), bf),
            pltpu.VMEM((B, T, sr, 2 * H), bf),
            pltpu.VMEM((B, R, H), bf),
            pltpu.VMEM((F, R, FD), bf),
            pltpu.VMEM((F, R, FD), bf),
            dma(6), dma(F), dma(F), dma(F), dma(F), dma(F), dma(F),
            dma(F * G), dma(G * T), dma(F * G), dma(G * T), dma(F * G), dma(G * T),
            dma(T), dma(T), dma(F), dma(F),
            dma(B * T), dma(B * T), dma(B * T), dma(B * T), dma(F), dma(F),
        ],
        compiler_params=pltpu.CompilerParams(collective_id=0, has_side_effects=True),
    )(
        tokens, routes.T, route_scores.T, norm_gain.reshape(1, Dz),
        jnp.swapaxes(expert_gate, 1, 2), jnp.swapaxes(expert_up, 1, 2), jnp.swapaxes(expert_down, 1, 2),
        shared_gate.T, shared_up.T, shared_down.T,
    )
    res = pl.pallas_call(
        write_kernel,
        out_shape=shapes,
        in_specs=[vm] * 7,
        out_specs=[hbm] * 7,
        scratch_shapes=[dma(7)],
    )(*res)
    return tuple(r[None] for r in res[:3]) + tuple(res[3:])


def dispatch(
    G, F, T,
    tokens, routes, route_scores, norm_gain,
    expert_gate, expert_up, expert_down, shared_gate, shared_up, shared_down,
):
    R, FD = tokens.shape
    E, Dz, Hs = expert_gate.shape
    args = (
        tokens, routes, route_scores, norm_gain,
        expert_gate, expert_up, expert_down, shared_gate, shared_up, shared_down,
    )
    dense = (
        F == T and E == F and Dz == FD and Hs % 16 == 0 and R == LANES
        and shared_gate.shape[1] == Hs and Dz % (LANES * G) == 0 and R % (16 * T) == 0
        and 2 * R * routes.shape[1] >= E * R
    )
    if dense:
        return fused(G, F, T, *args)
    return on_device(FD * T, Hs * T, shared_gate.shape[1] * T, *args)


def solution(mesh):
    in_specs = (
        P(("grp", "fs"), "tp"),
        P(("grp", "fs"), None),
        P(("grp", "fs"), None),
        P("fs"),
        P(None, "fs", "tp"),
        P(None, "fs", "tp"),
        P(None, "fs", "tp"),
        P("fs", "tp"),
        P("fs", "tp"),
        P("fs", "tp"),
    )
    out_specs = (
        P(("grp", "fs"), "tp", None),
        P(("grp", "fs"), "tp", None),
        P(("grp", "fs"), "tp", None),
        P(("grp", "tp"), None),
        P(("grp", "tp"), None),
        P(("grp", "tp"), None),
        P(("grp", "fs"), "tp"),
    )
    return jax.shard_map(
        functools.partial(dispatch, mesh.shape["grp"], mesh.shape["fs"], mesh.shape["tp"]),
        mesh=mesh,
        in_specs=in_specs,
        out_specs=out_specs,
        check_vma=False,
    )
```

```python
import functools

import jax
import jax.numpy as jnp
from jax import lax
from jax.experimental import pallas as pl
from jax.experimental.pallas import tpu as pltpu
from jax.sharding import PartitionSpec as P

LANES = 128
EPSILON = 1e-05
ROUTED_SCALE = 2.5


def on_device(
    model_width,
    hidden_units,
    shared_units,
    tokens,
    routes,
    route_scores,
    norm_gain,
    expert_gate,
    expert_up,
    expert_down,
    shared_gate,
    shared_up,
    shared_down,
):
    D, H, SH = model_width, hidden_units, shared_units
    gain_column = norm_gain[:, None]
    gate_rows, up_rows, down_rows = (
        lax.all_to_all(
            (expert_gate * gain_column[None]).astype(jnp.bfloat16),
            "fs",
            split_axis=0,
            concat_axis=1,
            tiled=True,
        ),
        lax.all_to_all(
            (expert_up * gain_column[None]).astype(jnp.bfloat16),
            "fs",
            split_axis=0,
            concat_axis=1,
            tiled=True,
        ),
        lax.all_to_all(
            expert_down.astype(jnp.bfloat16), "fs", split_axis=0, concat_axis=1, tiled=True
        ),
    )
    shared_gate_rows, shared_up_rows, shared_down_rows = (
        lax.all_gather((shared_gate * gain_column).astype(jnp.bfloat16), "fs", axis=0, tiled=True),
        lax.all_gather((shared_up * gain_column).astype(jnp.bfloat16), "fs", axis=0, tiled=True),
        lax.all_gather(shared_down.astype(jnp.bfloat16), "fs", axis=0, tiled=True),
    )
    served_gate, served_up, served_down, common_gate, common_up, common_down = (
        lax.all_to_all(gate_rows[0], "tp", split_axis=0, concat_axis=1, tiled=True),
        lax.all_to_all(up_rows[0], "tp", split_axis=0, concat_axis=1, tiled=True),
        lax.all_to_all(down_rows[0], "tp", split_axis=0, concat_axis=1, tiled=True),
        lax.all_to_all(shared_gate_rows, "tp", split_axis=0, concat_axis=1, tiled=True),
        lax.all_to_all(shared_up_rows, "tp", split_axis=0, concat_axis=1, tiled=True),
        lax.all_to_all(shared_down_rows, "tp", split_axis=0, concat_axis=1, tiled=True),
    )
    values = tokens.astype(jnp.float32)
    feature_sum, square_sum = lax.psum(
        (jnp.sum(values, axis=1), jnp.sum(values * values, axis=1)), "tp"
    )
    average = feature_sum / D
    variance = square_sum / D - average * average
    normed = ((values - average[:, None]) * lax.rsqrt(variance + EPSILON)[:, None]).astype(
        jnp.bfloat16
    )
    shared_gate_part = jnp.dot(normed, common_gate, preferred_element_type=jnp.float32) * D ** (
        -0.5
    )
    shared_up_part = jnp.dot(normed, common_up, preferred_element_type=jnp.float32) * D ** (-0.5)
    shared_gate_total, shared_up_total = (
        lax.psum(shared_gate_part.astype(jnp.bfloat16), "tp").astype(jnp.float32),
        lax.psum(shared_up_part.astype(jnp.bfloat16), "tp").astype(jnp.float32),
    )
    shared_hidden = (jax.nn.silu(shared_gate_total) * shared_up_total).astype(jnp.bfloat16)
    shared_part = jnp.einsum(
        "th,dh->td", shared_hidden, common_down, preferred_element_type=jnp.float32
    ) * SH ** (-0.5)
    tok_rows, top_count = routes.shape
    experts = expert_gate.shape[0]
    capacity = 2 * tok_rows * top_count // experts
    expert_ids = routes.reshape(-1)
    one_hot = (expert_ids[:, None] == jnp.arange(experts, dtype=jnp.int32)[None, :]).astype(
        jnp.int32
    )
    slot_rank = jnp.sum(jnp.cumsum(one_hot, axis=0) * one_hot, axis=1) - 1
    slot_index = expert_ids * capacity + slot_rank
    token_index = jnp.arange(expert_ids.shape[0], dtype=jnp.int32) // top_count
    slot_token = (
        jnp.full((experts * capacity,), tok_rows, jnp.int32).at[slot_index].set(token_index)
    )
    padded = jnp.concatenate([normed, jnp.zeros((1, normed.shape[1]), jnp.bfloat16)], axis=0)
    outgoing = padded[slot_token].reshape(experts, capacity, normed.shape[1])
    received = lax.all_to_all(outgoing, "fs", split_axis=0, concat_axis=0, tiled=True)
    gate_part = jnp.einsum(
        "scd,dh->sch", received, served_gate, preferred_element_type=jnp.float32
    ) * D ** (-0.5)
    up_part = jnp.einsum(
        "scd,dh->sch", received, served_up, preferred_element_type=jnp.float32
    ) * D ** (-0.5)
    gate_total = lax.psum(gate_part.astype(jnp.bfloat16), "tp").astype(jnp.float32)
    up_total = lax.psum(up_part.astype(jnp.bfloat16), "tp").astype(jnp.float32)
    hidden = (jax.nn.silu(gate_total) * up_total).astype(jnp.bfloat16)
    expert_out = jnp.einsum(
        "sch,dh->scd", hidden, served_down, preferred_element_type=jnp.float32
    ) * H ** (-0.5)
    returned = lax.all_to_all(
        expert_out.astype(jnp.bfloat16), "fs", split_axis=0, concat_axis=0, tiled=True
    )
    picked = returned.reshape(experts * capacity, returned.shape[2])[slot_index]
    picked = picked.reshape(tok_rows, top_count, returned.shape[2]).astype(jnp.float32)
    mix_weight = route_scores / jnp.sum(route_scores, axis=1, keepdims=True) * ROUTED_SCALE
    routed_part = jnp.sum(picked * mix_weight[:, :, None], axis=1)
    mixture = (shared_part + routed_part).astype(jnp.bfloat16)
    return (
        served_gate[None],
        served_up[None],
        served_down[None],
        common_gate,
        common_up,
        common_down,
        mixture,
    )


def fused_kernel(
    G, F, T, D, H,
    tok_in, routes, scores, gain, eg, eu, ed, sg, su, sd,
    o_sg, o_su, o_sd, o_cg, o_cu, o_cd, o_mix,
    tok, w32, sendg, sendd, sendc, sendf, zg, zd, zc, zf, we, de, wc, df,
    stat, tbuf, pbuf, rbuf, hbuf, obuf, ret,
    l_sem, zg_s, zg_r, zd_s, zd_r, zc_s, zc_r, zf_s, zf_r, xg_s, xg_r, xd_s, xd_r, xc_s, xc_r, xf_s, xf_r,
    st_s, st_r, tk_s, tk_r, rs_s, rs_r, ag_s, ag_r, rt_s, rt_r,
):
    y, z, t = lax.axis_index("grp"), lax.axis_index("fs"), lax.axis_index("tp")
    E, Hs, Dz = eg.shape
    R, FD = tok_in.shape
    hr = Dz // G
    sr = R // T
    bf, f32 = jnp.bfloat16, jnp.float32

    def at(y2, z2, t2):
        return {"grp": y2, "fs": z2, "tp": t2}

    def rc(src, dst, ss, rs, dev):
        return pltpu.make_async_remote_copy(
            src_ref=src, dst_ref=dst, send_sem=ss, recv_sem=rs,
            device_id=dev, device_id_type=pl.DeviceIdType.MESH,
        )

    barrier = pltpu.get_barrier_semaphore()
    peers = [at(y, lax.rem(z + d, F), t) for d in range(1, F)]
    for dy in range(G):
        for dt in range(T):
            if dy or dt:
                peers.append(at(lax.rem(y + dy, G), z, lax.rem(t + dt, T)))
    for dev in peers:
        pl.semaphore_signal(barrier, inc=1, device_id=dev, device_id_type=pl.DeviceIdType.MESH)

    half = pl.ds(pl.multiple_of(y * hr, hr), hr)
    tok_load = pltpu.make_async_copy(tok_in, tok, l_sem.at[6])
    tok_load.start()
    loads = []
    for i, (ref, sref) in enumerate(((eg, sg), (eu, su), (ed, sd))):
        loads.append(pltpu.make_async_copy(ref.at[:, :, half], w32.at[i, pl.ds(0, E)], l_sem.at[2 * i]))
        loads.append(pltpu.make_async_copy(sref.at[:, half], w32.at[i, E], l_sem.at[2 * i + 1]))
    loads = [loads[0], loads[2], loads[4], loads[1], loads[3], loads[5]]
    for c in loads:
        c.start()

    tok_load.wait()
    x = tok[...].astype(f32)
    s1 = jnp.sum(x, axis=1, keepdims=True)
    s2 = jnp.sum(x * x, axis=1, keepdims=True)
    lane = lax.broadcasted_iota(jnp.int32, (R, LANES), 1)
    stat[t] = jnp.where(lane == 0, s1, jnp.where(lane == 1, s2, 0.0)).T[0:8]
    gain_row = gain[0:1, half]

    loads[0].wait()
    loads[1].wait()
    for e in range(E):
        sendg[e, 0] = (w32[0, e] * gain_row).astype(bf)
        sendg[e, 1] = (w32[1, e] * gain_row).astype(bf)

    pl.semaphore_wait(barrier, len(peers))
    sent = []
    for d in range(1, T):
        c = rc(stat.at[t], stat.at[t], st_s.at[d - 1], st_r.at[t], at(y, z, lax.rem(t + d, T)))
        c.start()
        sent.append(c)

    def spread(src_of, zb, ss, rr):
        for d in range(1, F):
            z2 = lax.rem(z + d, F)
            c = rc(src_of(z2), zb.at[z], ss.at[d - 1], rr.at[z], at(y, z2, t))
            c.start()
            sent.append(c)
        pltpu.make_async_copy(src_of(z), zb.at[z], rr.at[z]).start()

    spread(lambda e: sendg.at[e], zg, zg_s, zg_r)

    loads[2].wait()
    for e in range(E):
        sendd[e] = w32[2, e].astype(bf)
    spread(lambda e: sendd.at[e], zd, zd_s, zd_r)

    for d in range(1, T):
        t2 = lax.rem(t + d, T)
        pltpu.make_async_copy(stat.at[t2], stat.at[t2], st_r.at[t2]).wait()
    tot = stat[0]
    for i in range(1, T):
        tot = tot + stat[i]
    back = jnp.concatenate([tot, jnp.zeros((LANES - 8, R), f32)], axis=0).T
    average = back[:, 0:1] / D
    variance = back[:, 1:2] / D - average * average
    tbuf[z] = ((tok[...].astype(f32) - average) * lax.rsqrt(variance + EPSILON)).astype(bf)
    for d in range(1, F):
        c = rc(tbuf.at[z], tbuf.at[z], tk_s.at[d - 1], tk_r.at[z], at(y, lax.rem(z + d, F), t))
        c.start()
        sent.append(c)

    for c in loads[3:]:
        c.wait()
    sendc[0] = (w32[0, E] * gain_row).astype(bf)
    sendc[1] = (w32[1, E] * gain_row).astype(bf)
    sendf[...] = w32[2, E].astype(bf)

    held = []

    def forward(zb, place, zr, xs, xr):
        for d in range(F):
            f = lax.rem(z + F - d, F)
            pltpu.make_async_copy(zb.at[f], zb.at[f], zr.at[f]).wait()
            for dy in range(G):
                c = rc(
                    zb.at[f], place(y, t), xs.at[d * G + dy], xr.at[y * T + t],
                    at(lax.rem(y + dy, G), z, f),
                )
                if dy:
                    c.start()
                    sent.append(c)
                else:
                    own = pltpu.make_async_copy(zb.at[f], place(y, t), xr.at[y * T + t])
                    pl.when(f != t)(c.start)
                    pl.when(f == t)(own.start)
                    held.append((f != t, c))

    def arrived(place, xr):
        for ys in range(G):
            for tt in range(T):
                pltpu.make_async_copy(place(ys, tt), place(ys, tt), xr.at[ys * T + tt]).wait()

    def columns(ys):
        return pl.ds(pl.multiple_of(ys * hr, hr), hr)

    def at_e(ys, tt):
        return we.at[:, tt, :, columns(ys)]

    def at_d(ys, tt):
        return de.at[tt, :, columns(ys)]

    def at_c(ys, tt):
        return wc.at[:, tt, :, columns(ys)]

    def at_f(ys, tt):
        return df.at[tt, :, columns(ys)]

    def rows_of(i):
        return pl.ds(pl.multiple_of(i * sr, sr), sr)

    def first(s):
        if 0 < s < F:
            j = lax.rem(z + F - s, F)
            pltpu.make_async_copy(tbuf.at[j], tbuf.at[j], tk_r.at[j]).wait()
        else:
            j = z
        w = we[...] if s < F else wc[...]
        pbuf[s] = (
            lax.dot_general(
                tbuf[j], w.reshape(2 * H, FD), (((1,), (1,)), ((), ())), preferred_element_type=f32
            ) * D ** (-0.5)
        ).astype(bf)
        for d in range(1, T):
            t2 = lax.rem(t + d, T)
            c = rc(pbuf.at[s, rows_of(t2)], rbuf.at[s, t], rs_s.at[s * T + d], rs_r.at[s * T + t], at(y, z, t2))
            c.start()
            sent.append(c)

    def second(s):
        acc = pbuf[s, rows_of(t)].astype(f32)
        for d in range(1, T):
            t2 = lax.rem(t + d, T)
            pltpu.make_async_copy(rbuf.at[s, t2], rbuf.at[s, t2], rs_r.at[s * T + t2]).wait()
            acc = acc + rbuf[s, t2].astype(f32)
        gate, up = acc[:, 0:H], acc[:, H:]
        mine = hbuf.at[s, rows_of(t)]
        mine[...] = (gate / (1.0 + jnp.exp(-gate)) * up).astype(bf)
        for d in range(1, T):
            c = rc(mine, mine, ag_s.at[s * T + d], ag_r.at[s * T + t], at(y, z, lax.rem(t + d, T)))
            c.start()
            sent.append(c)

    def third(s):
        for d in range(1, T):
            t2 = lax.rem(t + d, T)
            theirs = hbuf.at[s, rows_of(t2)]
            pltpu.make_async_copy(theirs, theirs, ag_r.at[s * T + t2]).wait()
        w = de[...] if s < F else df[...]
        value = jnp.dot(hbuf[s], w.reshape(H, FD), preferred_element_type=f32) * H ** (-0.5)
        if s == F:
            return value
        if s == 0:
            ret[z] = value.astype(bf)
        else:
            obuf[s] = value.astype(bf)
            c = rc(obuf.at[s], ret.at[z], rt_s.at[s], rt_r.at[z], at(y, lax.rem(z + F - s, F), t))
            c.start()
            sent.append(c)

    forward(zg, at_e, zg_r, xg_s, xg_r)
    arrived(at_e, xg_r)
    first(0)
    forward(zd, at_d, zd_r, xd_s, xd_r)
    first(1)
    second(0)
    arrived(at_d, xd_r)
    second(1)
    third(0)
    for s in range(2, F):
        first(s)
        third(s - 1)
        if s == 2:
            spread(lambda e: sendc, zc, zc_s, zc_r)
        second(s)
    third(F - 1)
    spread(lambda e: sendf, zf, zf_s, zf_r)
    o_sg[...] = we[0].reshape(H, FD).T
    o_su[...] = we[1].reshape(H, FD).T
    o_sd[...] = de[...].reshape(H, FD).T
    forward(zc, at_c, zc_r, xc_s, xc_r)
    arrived(at_c, xc_r)
    first(F)
    o_cg[...] = wc[0].reshape(H, FD).T
    second(F)
    o_cu[...] = wc[1].reshape(H, FD).T
    forward(zf, at_f, zf_r, xf_s, xf_r)
    weight = scores[...] / jnp.sum(scores[...], axis=0, keepdims=True) * ROUTED_SCALE
    picked = routes[...]
    line = lax.broadcasted_iota(jnp.int32, (LANES, R), 0)
    shares = jnp.zeros((LANES, R), f32)
    for e in range(E):
        share = jnp.sum(jnp.where(picked == e, weight, 0.0), axis=0, keepdims=True)
        shares = jnp.where(line == e, share, shares)
    shares = shares.T
    arrived(at_f, xf_r)
    total = third(F)
    o_cd[...] = df[...].reshape(H, FD).T
    for d in range(1, F):
        z2 = lax.rem(z + d, F)
        pltpu.make_async_copy(ret.at[z2], ret.at[z2], rt_r.at[z2]).wait()
    for e in range(E):
        total = total + shares[:, e:e + 1] * ret[e].astype(f32)
    o_mix[...] = total.astype(bf)

    for c in sent:
        c.wait_send()
    for other, c in held:
        pl.when(other)(c.wait_send)


def fused(
    G, F, T,
    tokens, routes, route_scores, norm_gain,
    expert_gate, expert_up, expert_down, shared_gate, shared_up, shared_down,
):
    R, FD = tokens.shape
    E, Dz, Hs = expert_gate.shape
    D, H = FD * T, Hs * T
    hr = Dz // G
    sr = R // T
    B = F + 1
    bf, f32 = jnp.bfloat16, jnp.float32
    vm, hbm = pl.BlockSpec(memory_space=pltpu.VMEM), pl.BlockSpec(memory_space=pl.ANY)
    dma = lambda n: pltpu.SemaphoreType.DMA((n,))
    weights = jax.ShapeDtypeStruct((FD, H), bf)
    shapes = [weights] * 6 + [jax.ShapeDtypeStruct((R, FD), bf)]
    res = pl.pallas_call(
        functools.partial(fused_kernel, G, F, T, D, H),
        out_shape=[pltpu.VMEM(s.shape, s.dtype) for s in shapes],
        in_specs=[hbm] + [vm] * 3 + [hbm] * 6,
        out_specs=[vm] * 7,
        scratch_shapes=[
            pltpu.VMEM((R, FD), bf),
            pltpu.VMEM((3, E + 1, Hs, hr), f32),
            pltpu.VMEM((E, 2, Hs, hr), bf),
            pltpu.VMEM((E, Hs, hr), bf),
            pltpu.VMEM((2, Hs, hr), bf),
            pltpu.VMEM((Hs, hr), bf),
            pltpu.VMEM((F, 2, Hs, hr), bf),
            pltpu.VMEM((F, Hs, hr), bf),
            pltpu.VMEM((F, 2, Hs, hr), bf),
            pltpu.VMEM((F, Hs, hr), bf),
            pltpu.VMEM((2, T, Hs, FD), bf),
            pltpu.VMEM((T, Hs, FD), bf),
            pltpu.VMEM((2, T, Hs, FD), bf),
            pltpu.VMEM((T, Hs, FD), bf),
            pltpu.VMEM((T, 8, R), f32),
            pltpu.VMEM((F, R, FD), bf),
            pltpu.VMEM((B, R, 2 * H), bf),
            pltpu.VMEM((B, T, sr, 2 * H), bf),
            pltpu.VMEM((B, R, H), bf),
            pltpu.VMEM((F, R, FD), bf),
            pltpu.VMEM((F, R, FD), bf),
            dma(7), dma(F), dma(F), dma(F), dma(F), dma(F), dma(F), dma(F), dma(F),
            dma(F * G), dma(G * T), dma(F * G), dma(G * T), dma(F * G), dma(G * T), dma(F * G), dma(G * T),
            dma(T), dma(T), dma(F), dma(F),
            dma(B * T), dma(B * T), dma(B * T), dma(B * T), dma(F), dma(F),
        ],
        compiler_params=pltpu.CompilerParams(collective_id=0, has_side_effects=True),
    )(
        tokens, routes.T, route_scores.T, norm_gain.reshape(1, Dz),
        jnp.swapaxes(expert_gate, 1, 2), jnp.swapaxes(expert_up, 1, 2), jnp.swapaxes(expert_down, 1, 2),
        shared_gate.T, shared_up.T, shared_down.T,
    )
    return tuple(r[None] for r in res[:3]) + tuple(res[3:])


def dispatch(
    G, F, T,
    tokens, routes, route_scores, norm_gain,
    expert_gate, expert_up, expert_down, shared_gate, shared_up, shared_down,
):
    R, FD = tokens.shape
    E, Dz, Hs = expert_gate.shape
    args = (
        tokens, routes, route_scores, norm_gain,
        expert_gate, expert_up, expert_down, shared_gate, shared_up, shared_down,
    )
    dense = (
        F == T and E == F and Dz == FD and Hs % 16 == 0 and R == LANES
        and shared_gate.shape[1] == Hs and Dz % (LANES * G) == 0 and R % (16 * T) == 0
        and 2 * R * routes.shape[1] >= E * R
    )
    if dense:
        return fused(G, F, T, *args)
    return on_device(FD * T, Hs * T, shared_gate.shape[1] * T, *args)


def solution(mesh):
    in_specs = (
        P(("grp", "fs"), "tp"),
        P(("grp", "fs"), None),
        P(("grp", "fs"), None),
        P("fs"),
        P(None, "fs", "tp"),
        P(None, "fs", "tp"),
        P(None, "fs", "tp"),
        P("fs", "tp"),
        P("fs", "tp"),
        P("fs", "tp"),
    )
    out_specs = (
        P(("grp", "fs"), "tp", None),
        P(("grp", "fs"), "tp", None),
        P(("grp", "fs"), "tp", None),
        P(("grp", "tp"), None),
        P(("grp", "tp"), None),
        P(("grp", "tp"), None),
        P(("grp", "fs"), "tp"),
    )
    return jax.shard_map(
        functools.partial(dispatch, mesh.shape["grp"], mesh.shape["fs"], mesh.shape["tp"]),
        mesh=mesh,
        in_specs=in_specs,
        out_specs=out_specs,
        check_vma=False,
    )
```
